32 devices in a mesh: sp: 8 (over z, x), tp: 4 (over y, core).
Axes of the slice: x: 2, y: 2, z: 4, core: 2. Of those that a mesh axis runs over, the one named last changes fastest.
Arguments:
- wide_query: bfloat16 [4096, 1536], P('sp', 'tp'), may hold values from -6 to 6
- wide_key: bfloat16 [4096, 1536], P('sp', 'tp'), may hold values from -6 to 6
- wide_value: bfloat16 [4096, 1536], P('sp', 'tp'), may hold values from -6 to 6
- wide_gate: bfloat16 [4096, 1536], P('sp', 'tp'), may hold values from -6 to 6
- narrow_query: bfloat16 [4096, 512], P('sp', 'tp'), may hold values from -6 to 6
- narrow_key: bfloat16 [4096, 512], P('sp', 'tp'), may hold values from -6 to 6
- narrow_value: bfloat16 [4096, 512], P('sp', 'tp'), may hold values from -6 to 6
- narrow_gate: bfloat16 [4096, 512], P('sp', 'tp'), may hold values from -6 to 6
- wide_decay: float32 [12, 4096], P('tp', 'sp'), may hold values from -1 to 0
- narrow_decay: float32 [8, 4096], P('tp', 'sp'), may hold values from -1 to 0
- residual: bfloat16 [4096, 2048], P(('sp', 'tp')), may hold values from -6 to 6
- wide_out: bfloat16 [1536, 2048], P('tp'), may hold values from -0.125 to 0.125
- narrow_out: bfloat16 [512, 2048], P('tp'), may hold values from -0.125 to 0.125
- up_weight: bfloat16 [2048, 8192], P('sp', 'tp'), may hold values from -0.125 to 0.125
- down_weight: bfloat16 [8192, 2048], P('tp', 'sp'), may hold values from -0.0625 to 0.0625
- gain_mix: float32 [2048], replicated, may hold values from 0.1 to 1.9
- gain_pre: float32 [2048], replicated, may hold values from 0.1 to 1.9
- gain_mlp: float32 [2048], replicated, may hold values from 0.1 to 1.9
Outputs:
- result: bfloat16 [4096, 2048], P(('sp', 'tp'))
The draws below stay inside these ranges and needn't reach their ends.
All inputs are finite; a program needn't handle non-finite values.
Results may differ from the reference program's by a relative error of at most 0.02.
Values may be sent and summed in bfloat16 or wider, within the bound.
A program may use at most 128 MiB of HBM per device.

```python
import math
import jax
import jax.numpy as jnp
from jax import lax

D = 2048
FF = 8192
WIDE_HEADS = 12
WIDE_DIM = 128
NARROW_HEADS = 8
NARROW_DIM = 64
SPAN = 128
TOK_DEV = 512
TOKEN_POSITIONS = 4096


def decay_law(source, count_of_heads):
    key_sequences = jax.random.split(source, 7)
    order = jax.random.permutation(key_sequences[0], count_of_heads)
    quick = order < count_of_heads // 2
    quick_rate = jnp.exp(jax.random.uniform(key_sequences[1], (count_of_heads,), jnp.float32, math.log(1.0 / 50.0), math.log(1.0 / 30.0)))
    slow_rate = jnp.exp(jax.random.uniform(key_sequences[2], (count_of_heads,), jnp.float32, math.log(0.12), math.log(0.35))) / TOKEN_POSITIONS
    base_rate = jnp.where(quick, quick_rate, slow_rate)
    block_count = TOKEN_POSITIONS // TOK_DEV
    factor = jnp.exp(jax.random.uniform(key_sequences[3], (count_of_heads, block_count), jnp.float32, math.log(0.5), math.log(2.0)))
    factor = jnp.repeat(factor, TOK_DEV, axis=1)
    jitter = jnp.exp(jax.random.uniform(key_sequences[4], (count_of_heads, TOKEN_POSITIONS), jnp.float32, math.log(0.6), math.log(1.4)))
    decay_rates = base_rate[:, None] * factor * jitter
    group_start_index = jax.random.randint(key_sequences[5], (count_of_heads, 2), 0, TOKEN_POSITIONS)
    group_length = jax.random.uniform(key_sequences[6], (count_of_heads, 2), jnp.float32, math.log(0.6), math.log(0.8))
    token_positions = jnp.arange(TOKEN_POSITIONS, dtype=jnp.int32)
    token_groups = jnp.sum(jnp.where(token_positions[None, None, :] == group_start_index[:, :, None], group_length[:, :, None], 0.0), axis=1)
    return (token_groups - decay_rates).astype(jnp.float32)


def draw_wide_decay(key, part):
    return decay_law(jax.random.fold_in(key, 11), WIDE_HEADS)


def draw_narrow_decay(key, part):
    return decay_law(jax.random.fold_in(key, 12), NARROW_HEADS)


def shard_levels(key, dims, shards, least, largest):
    def one(position, blocks):
        steps = jax.random.uniform(jax.random.fold_in(jax.random.fold_in(key, 6), position), (blocks,), jnp.float32, least / len(shards), largest / len(shards))
        return jnp.repeat(jnp.exp(steps), dims[position] // blocks).reshape((-1,) + (1,) * (len(dims) - position - 1))

    factor_of = one(*shards[0])
    for cut in shards[1:]:
        factor_of = factor_of * one(*cut)
    return factor_of


def gaussian(own_key, shape, deviation, reach, pieces=(), held_as=jnp.bfloat16):
    array = jax.random.normal(own_key, shape, jnp.float32) * deviation
    if len(pieces) > 0:
        array = shard_levels(own_key, shape, pieces, -0.22, 0.18) * array
    return jnp.clip(array, min=-reach, max=reach).astype(held_as)


def setup_inputs(seed: int = 0) -> dict:
    arg_keys = jax.random.split(jax.random.key(seed), 19)
    wide_query = gaussian(arg_keys[0], (TOKEN_POSITIONS, WIDE_HEADS * WIDE_DIM), 1.0, 6.0, ((0, 8), (1, 4)))
    wide_key = gaussian(arg_keys[1], (TOKEN_POSITIONS, WIDE_HEADS * WIDE_DIM), 1.0, 6.0, ((0, 8), (1, 4)))
    wide_value = gaussian(arg_keys[2], (TOKEN_POSITIONS, WIDE_HEADS * WIDE_DIM), 1.0, 6.0, ((0, 8), (1, 4)))
    wide_gate = gaussian(arg_keys[3], (TOKEN_POSITIONS, WIDE_HEADS * WIDE_DIM), 1.0, 6.0, ((0, 8), (1, 4)))
    narrow_query = gaussian(arg_keys[4], (TOKEN_POSITIONS, NARROW_HEADS * NARROW_DIM), 1.0, 6.0, ((0, 8), (1, 4)))
    narrow_key = gaussian(arg_keys[5], (TOKEN_POSITIONS, NARROW_HEADS * NARROW_DIM), 1.0, 6.0, ((0, 8), (1, 4)))
    narrow_value = gaussian(arg_keys[6], (TOKEN_POSITIONS, NARROW_HEADS * NARROW_DIM), 1.0, 6.0, ((0, 8), (1, 4)))
    narrow_gate = gaussian(arg_keys[7], (TOKEN_POSITIONS, NARROW_HEADS * NARROW_DIM), 1.0, 6.0, ((0, 8), (1, 4)))
    wide_decay = draw_wide_decay(jax.random.fold_in(arg_keys[18], 71), 0)
    narrow_decay = draw_narrow_decay(jax.random.fold_in(arg_keys[18], 71), 0)
    residual = gaussian(arg_keys[10], (TOKEN_POSITIONS, D), 1.0, 6.0, ((0, 32),))
    wide_out = gaussian(arg_keys[11], (WIDE_HEADS * WIDE_DIM, D), D ** -0.5, 0.125, ((0, 4),))
    narrow_out = gaussian(arg_keys[12], (NARROW_HEADS * NARROW_DIM, D), D ** -0.5, 0.125, ((0, 4),))
    up_weight = gaussian(arg_keys[13], (D, FF), D ** -0.5, 0.125, ((0, 8), (1, 4)))
    down_weight = gaussian(arg_keys[14], (FF, D), FF ** -0.5, 0.0625, ((0, 4), (1, 8)))
    gain_mix = jnp.clip(1.0 + 0.18 * jax.random.normal(arg_keys[15], (D,), jnp.float32), 0.1, 1.9)
    gain_pre = jnp.clip(1.0 + 0.18 * jax.random.normal(arg_keys[16], (D,), jnp.float32), 0.1, 1.9)
    gain_mlp = jnp.clip(1.0 + 0.18 * jax.random.normal(arg_keys[17], (D,), jnp.float32), 0.1, 1.9)
    return {"wide_query": wide_query, "wide_key": wide_key, "wide_value": wide_value, "wide_gate": wide_gate, "narrow_query": narrow_query, "narrow_key": narrow_key, "narrow_value": narrow_value, "narrow_gate": narrow_gate, "wide_decay": wide_decay, "narrow_decay": narrow_decay, "residual": residual, "wide_out": wide_out, "narrow_out": narrow_out, "up_weight": up_weight, "down_weight": down_weight, "gain_mix": gain_mix, "gain_pre": gain_pre, "gain_mlp": gain_mlp}


epsilon = 1e-06

def rotate(packed, head_dim, positions):
    length = packed.shape[0]
    grouped = packed.astype(jnp.float32).reshape(length, -1, head_dim)
    halfway = head_dim // 2
    inverse = 10000.0 ** (-jnp.arange(0, head_dim, 2, dtype=jnp.float32) / head_dim)
    angles = positions.astype(jnp.float32)[:, None] * inverse[None, :]
    cosine_table = jnp.cos(angles)[:, None, :]
    sine_table = jnp.sin(angles)[:, None, :]
    leading = grouped[..., :halfway]
    trailing = grouped[..., halfway:]
    return jnp.concatenate([leading * cosine_table - trailing * sine_table, leading * sine_table + trailing * cosine_table], axis=-1)

def rms_scale(values, gain_vector):
    return values * lax.rsqrt(lax.optimization_barrier(jnp.mean(values * values, axis=-1, keepdims=True)) + epsilon) * gain_vector.astype(jnp.float32)

def retention(query, key, value, gate, log_decay, head_dim):
    length = query.shape[0]
    count_of_heads = query.shape[1] // head_dim
    span_count = length // SPAN
    positions = jnp.arange(length, dtype=jnp.int32)
    queries = lax.optimization_barrier(rotate(query, head_dim, positions).astype(jnp.bfloat16))
    keys_full = rotate(key, head_dim, positions) * head_dim ** (-0.5)
    keys_half = lax.optimization_barrier(keys_full.astype(jnp.bfloat16))
    shaped = (span_count, SPAN, count_of_heads, head_dim)
    cumulative = jnp.cumsum(log_decay.T.reshape(span_count, SPAN, count_of_heads), axis=1)
    causal = jnp.arange(SPAN)[:, None] >= jnp.arange(SPAN)[None, :]

    def advance(carried, inputs):
        span_queries, span_keys, span_full, span_values, span_decay = inputs
        scores = jnp.einsum('ihd,jhd->hij', span_queries.astype(jnp.float32), span_keys.astype(jnp.float32), precision=lax.Precision.HIGHEST)
        decay_rows = span_decay.T
        log_gaps = jnp.where(causal[None], decay_rows[:, :, None] - decay_rows[:, None, :], -jnp.inf)
        weights = lax.optimization_barrier((scores * jnp.exp(log_gaps)).astype(jnp.bfloat16))
        within = jnp.einsum('hij,jhd->ihd', weights.astype(jnp.float32), span_values.astype(jnp.float32), precision=lax.Precision.HIGHEST)
        entering = lax.optimization_barrier(carried.astype(jnp.bfloat16)).astype(jnp.float32)
        across = jnp.einsum('ihd,hde->ihe', span_queries.astype(jnp.float32), entering, precision=lax.Precision.HIGHEST) * jnp.exp(span_decay)[:, :, None]
        span_total = span_decay[-1]
        scaled = lax.optimization_barrier((span_full * jnp.exp(span_total[None, :] - span_decay)[:, :, None]).astype(jnp.bfloat16))
        update = jnp.einsum('jhd,jhe->hde', scaled.astype(jnp.float32), span_values.astype(jnp.float32), precision=lax.Precision.HIGHEST)
        carried = carried * jnp.exp(span_total)[:, None, None] + update
        return (carried, within + across)
    initial = jnp.zeros((count_of_heads, head_dim, head_dim), jnp.float32)
    inputs = (queries.reshape(shaped), keys_half.reshape(shaped), keys_full.reshape(shaped), value.reshape(shaped), cumulative)
    closing, output = lax.scan(advance, initial, inputs)
    output = output.reshape(length, count_of_heads, head_dim)
    normed = output * lax.rsqrt(lax.optimization_barrier(jnp.mean(output * output, axis=-1, keepdims=True)) + epsilon)
    return (normed.reshape(length, -1) * jax.nn.silu(gate.astype(jnp.float32))).astype(jnp.bfloat16)

def reference(wide_query, wide_key, wide_value, wide_gate, narrow_query, narrow_key, narrow_value, narrow_gate, wide_decay, narrow_decay, residual, wide_out, narrow_out, up_weight, down_weight, gain_mix, gain_pre, gain_mlp):
    wide_mixed = retention(wide_query, wide_key, wide_value, wide_gate, wide_decay, WIDE_DIM)
    narrow_mixed = retention(narrow_query, narrow_key, narrow_value, narrow_gate, narrow_decay, NARROW_DIM)
    projected = jnp.dot(wide_mixed, wide_out, preferred_element_type=jnp.float32) + jnp.dot(narrow_mixed, narrow_out, preferred_element_type=jnp.float32)
    updated = (residual.astype(jnp.float32) + rms_scale(projected, gain_mix)).astype(jnp.bfloat16)
    normed = rms_scale(updated.astype(jnp.float32), gain_pre).astype(jnp.bfloat16)
    rectified = jax.nn.relu(jnp.dot(normed, up_weight, preferred_element_type=jnp.float32))
    hidden = (rectified * rectified).astype(jnp.bfloat16)
    lowered = jnp.dot(hidden, down_weight, preferred_element_type=jnp.float32)
    return (updated.astype(jnp.float32) + rms_scale(lowered, gain_mlp)).astype(jnp.bfloat16)
```

```python
import functools

import jax
import jax.numpy as jnp
from jax import lax
from jax.experimental import pallas as pl
from jax.experimental.pallas import tpu as pltpu
from jax.sharding import PartitionSpec as P

MESH = pl.DeviceIdType.MESH

WIDE_DIM = 128
NARROW_DIM = 64
SPAN = 128


epsilon = 1e-06


def pack_states(items):
    wide_decay, wide_state, narrow_decay, narrow_state = items
    decays = jnp.concatenate([wide_decay, narrow_decay])
    decays = jnp.pad(decays[None, :], ((0, 15), (0, 128 - decays.shape[0])))
    return jnp.concatenate(
        [wide_state.reshape(-1, 128), narrow_state.reshape(-1, 128), decays], axis=0
    ).astype(jnp.bfloat16)


def unpack_states(packed, like):
    packed = packed.astype(jnp.float32)
    wide_rows, narrow_rows = like[1].size // 128, like[3].size // 128
    decays = packed[wide_rows + narrow_rows]
    wide_heads, narrow_heads = like[0].shape[0], like[2].shape[0]
    return (
        decays[:wide_heads],
        packed[:wide_rows].reshape(like[1].shape),
        decays[wide_heads : wide_heads + narrow_heads],
        packed[wide_rows : wide_rows + narrow_rows].reshape(like[3].shape),
    )


def earlier_states(own, axis, count):
    whole, before, distance = own, None, 1
    while distance < count:
        arrived = lax.ppermute(
            pack_states(whole), axis, [(i, i + distance) for i in range(count - distance)]
        )
        arrived = unpack_states(arrived, own)
        before = arrived if before is None else combine_states(arrived, before)
        whole = combine_states(arrived, whole)
        distance *= 2
    return before


def rotate(packed, head_dim, positions):
    length = packed.shape[0]
    grouped = packed.astype(jnp.float32).reshape(length, -1, head_dim)
    halfway = head_dim // 2
    inverse = 10000.0 ** (-jnp.arange(0, head_dim, 2, dtype=jnp.float32) / head_dim)
    angles = positions.astype(jnp.float32)[:, None] * inverse[None, :]
    cosine_table = jnp.cos(angles)[:, None, :]
    sine_table = jnp.sin(angles)[:, None, :]
    leading = grouped[..., :halfway]
    trailing = grouped[..., halfway:]
    return jnp.concatenate(
        [
            leading * cosine_table - trailing * sine_table,
            leading * sine_table + trailing * cosine_table,
        ],
        axis=-1,
    )


def rms_scale(values, gain_vector):
    return (
        values
        * lax.rsqrt(jnp.mean(values * values, axis=-1, keepdims=True) + epsilon)
        * gain_vector
    )


def span_terms(query, key, value, log_decay, head_dim, offset):
    length = query.shape[0]
    count_of_heads = query.shape[1] // head_dim
    span_count = length // SPAN
    shaped = (span_count, SPAN, count_of_heads, head_dim)
    positions = offset + jnp.arange(length, dtype=jnp.int32)
    queries = rotate(query, head_dim, positions).astype(jnp.bfloat16).reshape(shaped)
    keys_full = (rotate(key, head_dim, positions) * head_dim ** (-0.5)).reshape(shaped)
    keys_half = keys_full.astype(jnp.bfloat16)
    values_all = value.reshape(shaped)
    cumulative = jnp.cumsum(log_decay.T.reshape(span_count, SPAN, count_of_heads), axis=1)
    causal = jnp.arange(SPAN)[:, None] >= jnp.arange(SPAN)[None, :]
    scores = jnp.einsum("nihd,njhd->nhij", queries, keys_half, preferred_element_type=jnp.float32)
    decay_rows = cumulative.transpose(0, 2, 1)
    log_gaps = jnp.where(causal, decay_rows[..., :, None] - decay_rows[..., None, :], -jnp.inf)
    weights = (scores * jnp.exp(log_gaps)).astype(jnp.bfloat16)
    within = jnp.einsum("nhij,njhd->nihd", weights, values_all, preferred_element_type=jnp.float32)
    span_total = cumulative[:, -1, :]
    scaled = (keys_full * jnp.exp(span_total[:, None, :] - cumulative)[..., None]).astype(
        jnp.bfloat16
    )
    own_state = jnp.einsum(
        "njhd,njhe->nhde", scaled, values_all, preferred_element_type=jnp.float32
    )

    def advance(carried, inputs):
        decay_sum, contribution = inputs
        return (carried * jnp.exp(decay_sum)[:, None, None] + contribution, carried)

    initial = jnp.zeros((count_of_heads, head_dim, head_dim), jnp.float32)
    closing, before = lax.scan(advance, initial, (span_total, own_state), unroll=True)
    device_decay = jnp.exp(jnp.sum(span_total, axis=0))
    return (queries, cumulative, within, span_total, before, closing, device_decay)


def finish(parts, prefix, gate, head_dim):
    queries, cumulative, within, span_total, before, closing, device_decay = parts
    length = gate.shape[0]
    earlier = jnp.cumsum(span_total, axis=0) - span_total
    entering = (prefix[None] * jnp.exp(earlier)[:, :, None, None] + before).astype(jnp.bfloat16)
    across = (
        jnp.einsum("nihd,nhde->nihe", queries, entering, preferred_element_type=jnp.float32)
        * jnp.exp(cumulative)[..., None]
    )
    output = (within + across).reshape(length, -1, head_dim)
    normed = output * lax.rsqrt(jnp.mean(output * output, axis=-1, keepdims=True) + epsilon)
    return (normed.reshape(length, -1) * jax.nn.silu(gate.astype(jnp.float32))).astype(jnp.bfloat16)


def combine_states(former, latter):
    return (
        former[0] * latter[0],
        former[1] * latter[0][:, None, None] + latter[1],
        former[2] * latter[2],
        former[3] * latter[2][:, None, None] + latter[3],
    )


def local(
    wide_query,
    wide_key,
    wide_value,
    wide_gate,
    narrow_query,
    narrow_key,
    narrow_value,
    narrow_gate,
    wide_decay,
    narrow_decay,
    residual,
    wide_out,
    narrow_out,
    up_weight,
    down_weight,
    gain_mix,
    gain_pre,
    gain_mlp,
):
    length = wide_query.shape[0]
    offset = lax.axis_index("sp") * length
    wide_parts = span_terms(wide_query, wide_key, wide_value, wide_decay, WIDE_DIM, offset)
    narrow_parts = span_terms(
        narrow_query, narrow_key, narrow_value, narrow_decay, NARROW_DIM, offset
    )
    prefixes = earlier_states(
        (wide_parts[6], wide_parts[5], narrow_parts[6], narrow_parts[5]),
        "sp",
        lax.axis_size("sp"),
    )
    wide_mixed = finish(wide_parts, prefixes[1], wide_gate, WIDE_DIM)
    narrow_mixed = finish(narrow_parts, prefixes[3], narrow_gate, NARROW_DIM)
    columns = down_weight.shape[1]
    count_sp, count_tp = lax.axis_size("sp"), lax.axis_size("tp")
    if columns % 128 == 0 and count_sp % 2 == 0 and count_sp >= 4 and count_tp > 1:
        up_whole = lax.all_gather(up_weight, "sp", axis=0, tiled=True)
        return tail_call(
            wide_mixed, narrow_mixed, wide_out, narrow_out, residual,
            gain_mix, gain_pre, gain_mlp, up_whole, down_weight, count_sp, count_tp,
        )
    return tail_plain(
        wide_mixed, narrow_mixed, wide_out, narrow_out, residual,
        gain_mix, gain_pre, gain_mlp, up_weight, down_weight,
    )


def tail_plain(
    wide_mixed, narrow_mixed, wide_out, narrow_out, residual,
    gain_mix, gain_pre, gain_mlp, up_weight, down_weight,
):
    wide_rows, narrow_rows = (
        lax.all_to_all(wide_mixed, "tp", split_axis=0, concat_axis=1, tiled=True),
        lax.all_to_all(narrow_mixed, "tp", split_axis=0, concat_axis=1, tiled=True),
    )
    wide_whole, narrow_whole = (
        lax.all_gather(wide_out, "tp", axis=0, tiled=True),
        lax.all_gather(narrow_out, "tp", axis=0, tiled=True),
    )
    projected = jnp.dot(wide_rows, wide_whole, preferred_element_type=jnp.float32) + jnp.dot(
        narrow_rows, narrow_whole, preferred_element_type=jnp.float32
    )
    updated = (residual.astype(jnp.float32) + rms_scale(projected, gain_mix)).astype(jnp.bfloat16)
    normed = rms_scale(updated.astype(jnp.float32), gain_pre).astype(jnp.bfloat16)
    block_rows = lax.all_gather(normed, "tp", axis=0, tiled=True)
    rectified = jax.nn.relu(
        jnp.dot(
            block_rows,
            lax.all_gather(up_weight, "sp", axis=0, tiled=True),
            preferred_element_type=jnp.float32,
        )
    )
    hidden = (rectified * rectified).astype(jnp.bfloat16)
    partial_terms = jnp.dot(
        hidden,
        lax.all_gather(down_weight, "sp", axis=1, tiled=True),
        preferred_element_type=jnp.float32,
    )
    lowered = lax.psum_scatter(
        partial_terms.astype(jnp.bfloat16), "tp", scatter_dimension=0, tiled=True
    ).astype(jnp.float32)
    return (updated.astype(jnp.float32) + rms_scale(lowered, gain_mlp)).astype(jnp.bfloat16)


PIECES = 2


def tail_kernel(
    count_sp, count_tp,
    wide_mixed, narrow_mixed, wide_out, narrow_out, residual,
    gain_mix, gain_pre, gain_mlp, up_hbm, down_hbm, result,
    up_held, slots, part_out, part_in, rows, hidden, low_out, low_in, updated, lowered,
    line_send, line_recv, pair_send, pair_recv, part_send, part_recv,
    row_send, row_recv, low_send, low_recv, local_sem,
):
    line = count_sp // 2
    sp, tp = lax.axis_index("sp"), lax.axis_index("tp")
    a, b = sp // 2, lax.rem(sp, 2)
    block_rows = residual.shape[0]
    length, features = rows.shape
    depth, columns = slots.shape[1], slots.shape[2]
    piece = depth // PIECES

    def at(line_place, pair_place):
        return (line_place * 2 + pair_place, tp)

    def peer(offset):
        return (sp, lax.rem(tp + offset, count_tp))

    own_down = pltpu.make_async_copy(down_hbm, slots.at[sp], local_sem.at[0])
    own_down.start()
    load_up = pltpu.make_async_copy(up_hbm, up_held, local_sem.at[1])
    load_up.start()

    barrier = pltpu.get_barrier_semaphore()
    greeted = [at(lax.rem(a + 1, line), b), at(lax.rem(a + line - 1, line), b), at(a, 1 - b)]
    greeted += [peer(offset) for offset in range(1, count_tp)]
    for other in greeted:
        pl.semaphore_signal(barrier, inc=1, device_id=other, device_id_type=MESH)
    pl.semaphore_wait(barrier, len(greeted))
    own_down.wait()

    def chunk(place, index):
        return slots.at[place, pl.ds(index * piece, piece)]

    def right_copy(step, index, place):
        ref = chunk(place * 2 + b, index)
        return pltpu.make_async_remote_copy(
            src_ref=ref, dst_ref=ref,
            send_sem=line_send.at[0, step, index], recv_sem=line_recv.at[0, step, index],
            device_id=at(jnp.minimum(a + 1, line - 1), b), device_id_type=MESH,
        )

    def left_copy(step, index, place):
        ref = chunk(place * 2 + b, index)
        return pltpu.make_async_remote_copy(
            src_ref=ref, dst_ref=ref,
            send_sem=line_send.at[1, step, index], recv_sem=line_recv.at[1, step, index],
            device_id=at(jnp.maximum(a - 1, 0), b), device_id_type=MESH,
        )

    def pair_copy(index, place, column):
        ref = chunk(place * 2 + column, index)
        return pltpu.make_async_remote_copy(
            src_ref=ref, dst_ref=ref,
            send_sem=pair_send.at[place, index], recv_sem=pair_recv.at[place, index],
            device_id=at(a, 1 - b), device_id_type=MESH,
        )

    for index in range(PIECES):
        @pl.when(a + 1 < line)
        def _():
            right_copy(0, index, a).start()

        @pl.when(a >= 1)
        def _():
            left_copy(0, index, a).start()

        pair_copy(index, a, b).start()

    def relay(step):
        for index in range(PIECES):
            @pl.when(a - 1 - step >= 0)
            def _():
                place = a - 1 - step
                right_copy(step, index, place).wait_recv()

                @pl.when(a + 1 < line)
                def _():
                    right_copy(step + 1, index, place).start()

                pair_copy(index, place, b).start()

            @pl.when(a + 1 + step < line)
            def _():
                place = a + 1 + step
                left_copy(step, index, place).wait_recv()

                @pl.when(a >= 1)
                def _():
                    left_copy(step + 1, index, place).start()

                pair_copy(index, place, b).start()

    def project(start):
        taken = pl.ds(pl.multiple_of(start * block_rows, block_rows), block_rows)
        return jnp.dot(
            wide_mixed[taken, :], wide_out[...], preferred_element_type=jnp.float32
        ) + jnp.dot(narrow_mixed[taken, :], narrow_out[...], preferred_element_type=jnp.float32)

    def part_copy(offset):
        return pltpu.make_async_remote_copy(
            src_ref=part_out.at[offset], dst_ref=part_in.at[offset],
            send_sem=part_send.at[offset], recv_sem=part_recv.at[offset],
            device_id=peer(offset), device_id_type=MESH,
        )

    @pl.loop(1, count_tp)
    def _(offset):
        part_out[offset] = project(lax.rem(tp + offset, count_tp)).astype(jnp.bfloat16)
        part_copy(offset).start()

    lowered[...] = project(tp)
    for offset in range(1, count_tp):
        part_copy(offset).wait_recv()
        lowered[...] += part_in[offset].astype(jnp.float32)

    mine = pl.ds(pl.multiple_of(tp * block_rows, block_rows), block_rows)
    moved = residual[...].astype(jnp.float32) + rms_scale(lowered[...], gain_mix[...])
    moved = moved.astype(jnp.bfloat16)
    updated[...] = moved
    rows[mine, :] = rms_scale(moved.astype(jnp.float32), gain_pre[...]).astype(jnp.bfloat16)

    def row_copy(offset):
        return pltpu.make_async_remote_copy(
            src_ref=rows.at[mine], dst_ref=rows.at[mine],
            send_sem=row_send.at[offset], recv_sem=row_recv.at[offset],
            device_id=peer(offset), device_id_type=MESH,
        )

    for offset in range(1, count_tp):
        row_copy(offset).start()
    relay(0)
    load_up.wait()
    for offset in range(1, count_tp):
        row_copy(offset).wait_recv()

    width = 256

    @pl.loop(0, hidden.shape[1] // width)
    def _(tile):
        taken = pl.ds(pl.multiple_of(tile * width, width), width)
        rectified = jax.nn.relu(
            jnp.dot(rows[...], up_held[:, taken], preferred_element_type=jnp.float32)
        )
        hidden[:, taken] = (rectified * rectified).astype(jnp.bfloat16)

    def low_copy(offset, block):
        start = lax.rem(tp + offset, count_tp) * block_rows
        return pltpu.make_async_remote_copy(
            src_ref=low_out.at[block, pl.ds(pl.multiple_of(start, block_rows), block_rows)],
            dst_ref=low_in.at[offset, block],
            send_sem=low_send.at[offset, block], recv_sem=low_recv.at[offset, block],
            device_id=peer(offset), device_id_type=MESH,
        )

    def consume(block):
        low_out[block] = jnp.dot(
            hidden[...], slots[block], preferred_element_type=jnp.float32
        ).astype(jnp.bfloat16)
        for offset in range(1, count_tp):
            low_copy(offset, block).start()

    def at_distance(act, distance):
        @pl.when(a - distance >= 0)
        def _():
            act(a - distance)

        @pl.when((a + distance < line) & (distance > 0))
        def _():
            act(a + distance)

    def from_pair(place):
        for index in range(PIECES):
            pair_copy(index, place, 1 - b).wait_recv()
        consume(place * 2 + 1 - b)

    @pl.loop(0, line)
    def _(distance):
        @pl.when(distance + 1 <= line - 2)
        def _():
            relay(distance + 1)

        at_distance(lambda place: consume(place * 2 + b), distance)
        at_distance(from_pair, distance)

    for block in range(count_sp):
        taken = slice(block * columns, (block + 1) * columns)
        total = low_out[block, mine, :].astype(jnp.float32)
        for offset in range(1, count_tp):
            low_copy(offset, block).wait_recv()
            total += low_in[offset, block].astype(jnp.float32)
        lowered[:, taken] = total
    result[...] = (
        updated[...].astype(jnp.float32) + rms_scale(lowered[...], gain_mlp[...])
    ).astype(jnp.bfloat16)

    for offset in range(1, count_tp):
        part_copy(offset).wait_send()
        row_copy(offset).wait_send()

        @pl.loop(0, count_sp)
        def _(block):
            low_copy(offset, block).wait_send()

    for index in range(PIECES):
        @pl.loop(0, line)
        def _(place):
            pair_copy(index, place, b).wait_send()

        @pl.loop(0, line - 1)
        def _(step):
            @pl.when((a + 1 < line) & (a - step >= 0))
            def _():
                right_copy(step, index, jnp.maximum(a - step, 0)).wait_send()

            @pl.when((a >= 1) & (a + step < line))
            def _():
                left_copy(step, index, jnp.minimum(a + step, line - 1)).wait_send()


def tail_call(
    wide_mixed, narrow_mixed, wide_out, narrow_out, residual,
    gain_mix, gain_pre, gain_mlp, up_whole, down_weight, count_sp, count_tp,
):
    block_rows, features = residual.shape
    length = block_rows * count_tp
    depth, columns = down_weight.shape
    half, line = jnp.bfloat16, count_sp // 2
    dma = pltpu.SemaphoreType.DMA
    vmem = pl.BlockSpec(memory_space=pltpu.VMEM)
    anywhere = pl.BlockSpec(memory_space=pl.ANY)
    return pl.pallas_call(
        functools.partial(tail_kernel, count_sp, count_tp),
        out_shape=jax.ShapeDtypeStruct(residual.shape, half),
        in_specs=[vmem] * 8 + [anywhere] * 2,
        out_specs=vmem,
        scratch_shapes=[
            pltpu.VMEM(up_whole.shape, half),
            pltpu.VMEM((count_sp, depth, columns), half),
            pltpu.VMEM((count_tp, block_rows, features), half),
            pltpu.VMEM((count_tp, block_rows, features), half),
            pltpu.VMEM((length, features), half),
            pltpu.VMEM((length, depth), half),
            pltpu.VMEM((count_sp, length, columns), half),
            pltpu.VMEM((count_tp, count_sp, block_rows, columns), half),
            pltpu.VMEM((block_rows, features), half),
            pltpu.VMEM((block_rows, features), jnp.float32),
            dma((2, line - 1, PIECES)),
            dma((2, line - 1, PIECES)),
            dma((line, PIECES)),
            dma((line, PIECES)),
            dma((count_tp,)),
            dma((count_tp,)),
            dma((count_tp,)),
            dma((count_tp,)),
            dma((count_tp, count_sp)),
            dma((count_tp, count_sp)),
            dma((2,)),
        ],
        compiler_params=pltpu.CompilerParams(
            collective_id=0, has_side_effects=True, vmem_limit_bytes=52 * 1024 * 1024
        ),
    )(
        wide_mixed, narrow_mixed, wide_out, narrow_out, residual,
        gain_mix[None, :], gain_pre[None, :], gain_mlp[None, :], up_whole, down_weight,
    )


def solution(mesh):
    return jax.shard_map(
        local,
        mesh=mesh,
        in_specs=(
            P("sp", "tp"),
            P("sp", "tp"),
            P("sp", "tp"),
            P("sp", "tp"),
            P("sp", "tp"),
            P("sp", "tp"),
            P("sp", "tp"),
            P("sp", "tp"),
            P("tp", "sp"),
            P("tp", "sp"),
            P(("sp", "tp"), None),
            P("tp", None),
            P("tp", None),
            P("sp", "tp"),
            P("tp", "sp"),
            P(),
            P(),
            P(),
        ),
        out_specs=P(("sp", "tp"), None),
        check_vma=False,
    )
```

```python
import functools

import jax
import jax.numpy as jnp
from jax import lax
from jax.experimental import pallas as pl
from jax.experimental.pallas import tpu as pltpu
from jax.sharding import PartitionSpec as P

MESH = pl.DeviceIdType.MESH

WIDE_DIM = 128
NARROW_DIM = 64
SPAN = 128


epsilon = 1e-06


def pack_states(items):
    wide_decay, wide_state, narrow_decay, narrow_state = items
    decays = jnp.concatenate([wide_decay, narrow_decay])
    decays = jnp.pad(decays[None, :], ((0, 15), (0, 128 - decays.shape[0])))
    return jnp.concatenate(
        [wide_state.reshape(-1, 128), narrow_state.reshape(-1, 128), decays], axis=0
    ).astype(jnp.bfloat16)


def unpack_states(packed, like):
    packed = packed.astype(jnp.float32)
    wide_rows, narrow_rows = like[1].size // 128, like[3].size // 128
    decays = packed[wide_rows + narrow_rows]
    wide_heads, narrow_heads = like[0].shape[0], like[2].shape[0]
    return (
        decays[:wide_heads],
        packed[:wide_rows].reshape(like[1].shape),
        decays[wide_heads : wide_heads + narrow_heads],
        packed[wide_rows : wide_rows + narrow_rows].reshape(like[3].shape),
    )


def earlier_states(own, axis, count):
    whole, before, distance = own, None, 1
    while distance < count:
        arrived = lax.ppermute(
            pack_states(whole), axis, [(i, i + distance) for i in range(count - distance)]
        )
        arrived = unpack_states(arrived, own)
        before = arrived if before is None else combine_states(arrived, before)
        whole = combine_states(arrived, whole)
        distance *= 2
    return before


def rotate(packed, head_dim, positions):
    length = packed.shape[0]
    grouped = packed.astype(jnp.float32).reshape(length, -1, head_dim)
    halfway = head_dim // 2
    inverse = 10000.0 ** (-jnp.arange(0, head_dim, 2, dtype=jnp.float32) / head_dim)
    angles = positions.astype(jnp.float32)[:, None] * inverse[None, :]
    cosine_table = jnp.cos(angles)[:, None, :]
    sine_table = jnp.sin(angles)[:, None, :]
    leading = grouped[..., :halfway]
    trailing = grouped[..., halfway:]
    return jnp.concatenate(
        [
            leading * cosine_table - trailing * sine_table,
            leading * sine_table + trailing * cosine_table,
        ],
        axis=-1,
    )


def rms_scale(values, gain_vector):
    return (
        values
        * lax.rsqrt(jnp.mean(values * values, axis=-1, keepdims=True) + epsilon)
        * gain_vector
    )


def span_terms(query, key, value, log_decay, head_dim, offset):
    length = query.shape[0]
    count_of_heads = query.shape[1] // head_dim
    span_count = length // SPAN
    shaped = (span_count, SPAN, count_of_heads, head_dim)
    positions = offset + jnp.arange(length, dtype=jnp.int32)
    queries = rotate(query, head_dim, positions).astype(jnp.bfloat16).reshape(shaped)
    keys_full = (rotate(key, head_dim, positions) * head_dim ** (-0.5)).reshape(shaped)
    keys_half = keys_full.astype(jnp.bfloat16)
    values_all = value.reshape(shaped)
    cumulative = jnp.cumsum(log_decay.T.reshape(span_count, SPAN, count_of_heads), axis=1)
    causal = jnp.arange(SPAN)[:, None] >= jnp.arange(SPAN)[None, :]
    scores = jnp.einsum("nihd,njhd->nhij", queries, keys_half, preferred_element_type=jnp.float32)
    decay_rows = cumulative.transpose(0, 2, 1)
    log_gaps = jnp.where(causal, decay_rows[..., :, None] - decay_rows[..., None, :], -jnp.inf)
    weights = (scores * jnp.exp(log_gaps)).astype(jnp.bfloat16)
    within = jnp.einsum("nhij,njhd->nihd", weights, values_all, preferred_element_type=jnp.float32)
    span_total = cumulative[:, -1, :]
    scaled = (keys_full * jnp.exp(span_total[:, None, :] - cumulative)[..., None]).astype(
        jnp.bfloat16
    )
    own_state = jnp.einsum(
        "njhd,njhe->nhde", scaled, values_all, preferred_element_type=jnp.float32
    )

    def advance(carried, inputs):
        decay_sum, contribution = inputs
        return (carried * jnp.exp(decay_sum)[:, None, None] + contribution, carried)

    initial = jnp.zeros((count_of_heads, head_dim, head_dim), jnp.float32)
    closing, before = lax.scan(advance, initial, (span_total, own_state), unroll=True)
    device_decay = jnp.exp(jnp.sum(span_total, axis=0))
    return (queries, cumulative, within, span_total, before, closing, device_decay)


def finish(parts, prefix, gate, head_dim):
    queries, cumulative, within, span_total, before, closing, device_decay = parts
    length = gate.shape[0]
    earlier = jnp.cumsum(span_total, axis=0) - span_total
    entering = (prefix[None] * jnp.exp(earlier)[:, :, None, None] + before).astype(jnp.bfloat16)
    across = (
        jnp.einsum("nihd,nhde->nihe", queries, entering, preferred_element_type=jnp.float32)
        * jnp.exp(cumulative)[..., None]
    )
    output = (within + across).reshape(length, -1, head_dim)
    normed = output * lax.rsqrt(jnp.mean(output * output, axis=-1, keepdims=True) + epsilon)
    return (normed.reshape(length, -1) * jax.nn.silu(gate.astype(jnp.float32))).astype(jnp.bfloat16)


def combine_states(former, latter):
    return (
        former[0] * latter[0],
        former[1] * latter[0][:, None, None] + latter[1],
        former[2] * latter[2],
        former[3] * latter[2][:, None, None] + latter[3],
    )


def local(
    wide_query,
    wide_key,
    wide_value,
    wide_gate,
    narrow_query,
    narrow_key,
    narrow_value,
    narrow_gate,
    wide_decay,
    narrow_decay,
    residual,
    wide_out,
    narrow_out,
    up_weight,
    down_weight,
    gain_mix,
    gain_pre,
    gain_mlp,
):
    columns = down_weight.shape[1]
    count_sp, count_tp = lax.axis_size("sp"), lax.axis_size("tp")
    if (
        columns % 128 == 0 and count_sp % 4 == 0 and count_sp >= 8 and count_tp > 1
        and narrow_query.shape[1] % 128 == 0
    ):
        return whole_call(
            (wide_query, wide_key, wide_value, wide_gate),
            (narrow_query, narrow_key, narrow_value, narrow_gate),
            wide_decay, narrow_decay, residual, wide_out, narrow_out,
            up_weight, down_weight, gain_mix, gain_pre, gain_mlp, count_sp, count_tp,
        )
    length = wide_query.shape[0]
    offset = lax.axis_index("sp") * length
    wide_parts = span_terms(wide_query, wide_key, wide_value, wide_decay, WIDE_DIM, offset)
    narrow_parts = span_terms(
        narrow_query, narrow_key, narrow_value, narrow_decay, NARROW_DIM, offset
    )
    prefixes = earlier_states(
        (wide_parts[6], wide_parts[5], narrow_parts[6], narrow_parts[5]),
        "sp",
        lax.axis_size("sp"),
    )
    wide_mixed = finish(wide_parts, prefixes[1], wide_gate, WIDE_DIM)
    narrow_mixed = finish(narrow_parts, prefixes[3], narrow_gate, NARROW_DIM)
    return tail_plain(
        wide_mixed, narrow_mixed, wide_out, narrow_out, residual,
        gain_mix, gain_pre, gain_mlp, up_weight, down_weight,
    )


def tail_plain(
    wide_mixed, narrow_mixed, wide_out, narrow_out, residual,
    gain_mix, gain_pre, gain_mlp, up_weight, down_weight,
):
    wide_rows, narrow_rows = (
        lax.all_to_all(wide_mixed, "tp", split_axis=0, concat_axis=1, tiled=True),
        lax.all_to_all(narrow_mixed, "tp", split_axis=0, concat_axis=1, tiled=True),
    )
    wide_whole, narrow_whole = (
        lax.all_gather(wide_out, "tp", axis=0, tiled=True),
        lax.all_gather(narrow_out, "tp", axis=0, tiled=True),
    )
    projected = jnp.dot(wide_rows, wide_whole, preferred_element_type=jnp.float32) + jnp.dot(
        narrow_rows, narrow_whole, preferred_element_type=jnp.float32
    )
    updated = (residual.astype(jnp.float32) + rms_scale(projected, gain_mix)).astype(jnp.bfloat16)
    normed = rms_scale(updated.astype(jnp.float32), gain_pre).astype(jnp.bfloat16)
    block_rows = lax.all_gather(normed, "tp", axis=0, tiled=True)
    rectified = jax.nn.relu(
        jnp.dot(
            block_rows,
            lax.all_gather(up_weight, "sp", axis=0, tiled=True),
            preferred_element_type=jnp.float32,
        )
    )
    hidden = (rectified * rectified).astype(jnp.bfloat16)
    partial_terms = jnp.dot(
        hidden,
        lax.all_gather(down_weight, "sp", axis=1, tiled=True),
        preferred_element_type=jnp.float32,
    )
    lowered = lax.psum_scatter(
        partial_terms.astype(jnp.bfloat16), "tp", scatter_dimension=0, tiled=True
    ).astype(jnp.float32)
    return (updated.astype(jnp.float32) + rms_scale(lowered, gain_mlp)).astype(jnp.bfloat16)


PIECES = 2


def swap_halves(values, head_dim):
    half = head_dim // 2
    if head_dim == 128:
        return pltpu.roll(values, half, 1)
    lane = lax.broadcasted_iota(jnp.int32, values.shape, 1)
    return jnp.where(
        lax.rem(lane, head_dim) < half,
        pltpu.roll(values, 128 - half, 1),
        pltpu.roll(values, half, 1),
    )


def whole_kernel(
    count_sp, count_tp, wide_groups, narrow_groups,
    wide_query, wide_key, wide_value, wide_gate,
    narrow_query, narrow_key, narrow_value, narrow_gate,
    tables, cum_rows, cum_lanes, total_lanes, earlier_lanes, device_lanes,
    residual, wide_out, narrow_out, gain_mix, gain_pre, gain_mlp, up_hbm, down_hbm,
    result,
    up_slots, down_slots, part_out, part_in, rows, hidden, low_out, low_in, updated, lowered,
    turned, within, carried, mixed, state, prefix, prefix_decay, state_out, state_in,
    decay_out, decay_in,
    line_send, line_recv, pair_send, pair_recv, swap_send, swap_recv, part_send, part_recv,
    row_send, row_recv, low_send, low_recv, state_send, state_recv, decay_send, decay_recv,
    local_sem,
):
    line = count_sp // 2
    groups = wide_groups + narrow_groups
    sp, tp = lax.axis_index("sp"), lax.axis_index("tp")
    a, b = sp // 2, lax.rem(sp, 2)
    twin = a + 1 - 2 * lax.rem(a, 2)
    block_rows = residual.shape[0]
    length, features = rows.shape
    slots = (up_slots, down_slots)
    depth, columns = down_slots.shape[1], down_slots.shape[2]
    slab = up_slots.shape[1]
    half = jnp.bfloat16
    distances = []
    while 2 ** len(distances) < count_sp:
        distances.append(2 ** len(distances))

    def at(line_place, pair_place):
        return (line_place * 2 + pair_place, tp)

    def peer(offset):
        return (sp, lax.rem(tp + offset, count_tp))

    own_up = pltpu.make_async_copy(up_hbm, up_slots.at[sp], local_sem.at[0])
    own_up.start()
    own_down = pltpu.make_async_copy(down_hbm, down_slots.at[sp], local_sem.at[1])
    own_down.start()

    barrier = pltpu.get_barrier_semaphore()
    greeted = [at(a, 1 - b)]
    greeted += [(lax.rem(sp + step, count_sp), tp) for step in distances]
    greeted += [(lax.rem(sp + count_sp - step, count_sp), tp) for step in distances]
    greeted += [peer(offset) for offset in range(1, count_tp)]
    for other in greeted:
        pl.semaphore_signal(barrier, inc=1, device_id=other, device_id_type=MESH)
    pl.semaphore_wait(barrier, len(greeted))
    own_up.wait()
    own_down.wait()

    def chunk(which, place, index):
        piece = slots[which].shape[1] // PIECES
        return slots[which].at[place, pl.ds(index * piece, piece)]

    def remote(source, target, send, recv, device):
        return pltpu.make_async_remote_copy(
            src_ref=source, dst_ref=target, send_sem=send, recv_sem=recv,
            device_id=device, device_id_type=MESH,
        )

    def right_copy(which, step, index, place):
        ref = chunk(which, place * 2 + b, index)
        return remote(
            ref, ref, line_send.at[which, 0, step, index], line_recv.at[which, 0, step, index],
            at(jnp.minimum(a + 1, line - 1), b),
        )

    def left_copy(which, step, index, place):
        ref = chunk(which, place * 2 + b, index)
        return remote(
            ref, ref, line_send.at[which, 1, step, index], line_recv.at[which, 1, step, index],
            at(jnp.maximum(a - 1, 0), b),
        )

    def pair_copy(which, index, place, column):
        ref = chunk(which, place * 2 + column, index)
        return remote(
            ref, ref, pair_send.at[which, place, index], pair_recv.at[which, place, index],
            at(a, 1 - b),
        )

    def swap_copy(which, place):
        ref = chunk(which, place * 2 + 1 - b, 1)
        return remote(ref, ref, swap_send.at[which], swap_recv.at[which], at(twin, b))

    def begin(which):
        for index in range(PIECES):
            @pl.when(a + 1 < line)
            def _():
                right_copy(which, 0, index, a).start()

            @pl.when(a >= 1)
            def _():
                left_copy(which, 0, index, a).start()

            pair_copy(which, index, a, b).start()

    def to_pair(which, index, place):
        if index == 0:
            pair_copy(which, index, place, b).start()
        else:
            @pl.when(place != twin)
            def _():
                pair_copy(which, index, place, b).start()

    def relay(which, step, first):
        for index in range(PIECES):
            @pl.when(a - 1 - step >= 0)
            def _():
                place = a - 1 - step
                right_copy(which, step, index, place).wait_recv()

                @pl.when((a + 1 < line) & (step < line - 2))
                def _():
                    right_copy(which, jnp.minimum(step + 1, line - 2), index, place).start()

                to_pair(which, index, place)

            @pl.when(a + 1 + step < line)
            def _():
                place = a + 1 + step
                left_copy(which, step, index, place).wait_recv()

                @pl.when((a >= 1) & (step < line - 2))
                def _():
                    left_copy(which, jnp.minimum(step + 1, line - 2), index, place).start()

                to_pair(which, index, place)

        if first:
            pair_copy(which, 1, a, 1 - b).wait_recv()
            swap_copy(which, a).start()

    def wait_pair(which, place):
        pair_copy(which, 0, place, 1 - b).wait_recv()

        @pl.when((place != a) & (place != twin))
        def _():
            pair_copy(which, 1, place, 1 - b).wait_recv()

        @pl.when(place == twin)
        def _():
            swap_copy(which, place).wait_recv()

    begin(0)

    lane = lax.broadcasted_iota(jnp.int32, (SPAN, 128), 1)
    position = lax.broadcasted_iota(jnp.int32, (SPAN, 128), 0)
    causal = position >= lane
    low_half = lane < 64
    same_head = low_half == (position < 64)
    plans = [(g, False, g) for g in range(wide_groups)]
    plans += [(wide_groups + g, True, g) for g in range(narrow_groups)]

    def dot(left, right, left_dim, right_dim):
        return lax.dot_general(
            left, right, (((left_dim,), (right_dim,)), ((), ())),
            preferred_element_type=jnp.float32,
        )

    for g in range(groups):
        state[g] = jnp.zeros((128, 128), jnp.float32)

    @pl.loop(0, length // SPAN)
    def _(span):
        taken = pl.ds(pl.multiple_of(span * SPAN, SPAN), SPAN)
        for g, narrow, own in plans:
            lanes, mine = slice(g * 128, (g + 1) * 128), slice(own * 128, (own + 1) * 128)
            if narrow:
                query, key, value = narrow_query, narrow_key, narrow_value
                head_dim, cosine, sine = NARROW_DIM, tables[2, taken, :], tables[3, taken, :]
            else:
                query, key, value = wide_query, wide_key, wide_value
                head_dim, cosine, sine = WIDE_DIM, tables[0, taken, :], tables[1, taken, :]
            raw = query[taken, mine].astype(jnp.float32)
            spun = (raw * cosine + swap_halves(raw, head_dim) * sine).astype(half)
            turned[taken, lanes] = spun
            raw = key[taken, mine].astype(jnp.float32)
            full = (raw * cosine + swap_halves(raw, head_dim) * sine) * head_dim ** (-0.5)
            keys = full.astype(half)
            values = value[taken, mine]
            sums = cum_lanes[taken, lanes]
            total = total_lanes[pl.ds(pl.multiple_of(span * 8, 8), 8), lanes][0:1]

            def attend(queries, column, head):
                gaps = jnp.where(causal, column - cum_rows[head : head + 1, taken], -jnp.inf)
                weights = (dot(queries, keys, 1, 1) * jnp.exp(gaps)).astype(half)
                return dot(weights, values, 1, 0)

            if narrow:
                head = wide_groups + 2 * own
                first = attend(jnp.where(low_half, spun, jnp.zeros_like(spun)), sums[:, 0:1], head)
                second = attend(
                    jnp.where(low_half, jnp.zeros_like(spun), spun), sums[:, 64:65], head + 1
                )
                within[taken, lanes] = jnp.where(low_half, first, second)
            else:
                within[taken, lanes] = attend(spun, sums, g)
            scaled = (full * jnp.exp(total - sums)).astype(half)
            update = dot(scaled, values, 0, 0)
            if narrow:
                update = jnp.where(same_head, update, 0.0)
            old = state[g]
            carried[span, g] = old
            state[g] = old * jnp.exp(total) + update

    prefix[...] = jnp.zeros_like(prefix)
    prefix_decay[...] = jnp.ones_like(prefix_decay)

    def state_copies(step):
        device = (lax.rem(sp + distances[step], count_sp), tp)
        return (
            remote(
                state_out.at[step], state_in.at[step],
                state_send.at[step], state_recv.at[step], device,
            ),
            remote(
                decay_out.at[step], decay_in.at[step],
                decay_send.at[step], decay_recv.at[step], device,
            ),
        )

    def send_state(step):
        @pl.when(sp + distances[step] < count_sp)
        def _():
            for copy in state_copies(step):
                copy.start()

    def take_state(step):
        @pl.when(sp >= distances[step])
        def _():
            for copy in state_copies(step):
                copy.wait_recv()
            for g in range(groups):
                arrived = state_in[step, g].astype(jnp.float32)
                decay = decay_in[step, g : g + 1, :]
                prefix[g] = arrived * prefix_decay[g : g + 1, :] + prefix[g]
                prefix_decay[g : g + 1, :] = decay * prefix_decay[g : g + 1, :]
                if step + 1 < len(distances):
                    mine = decay_out[step, g : g + 1, :]
                    state[g] = arrived * mine + state[g]
                    decay_out[step + 1, g : g + 1, :] = decay * mine
                    state_out[step + 1, g] = state[g].astype(half)

        if step + 1 < len(distances):
            @pl.when(sp < distances[step])
            def _():
                decay_out[step + 1] = decay_out[step]
                for g in range(groups):
                    state_out[step + 1, g] = state[g].astype(half)

            send_state(step + 1)

    decay_out[0] = jnp.ones_like(decay_out[0])
    for g in range(groups):
        decay_out[0, g : g + 1, :] = device_lanes[:, g * 128 : (g + 1) * 128]
        state_out[0, g] = state[g].astype(half)
    send_state(0)
    relay(0, 0, True)
    begin(1)
    for step in range(max(len(distances), line - 1)):
        if step < len(distances):
            take_state(step)
        if step + 1 <= line - 2:
            relay(0, step + 1, False)
        elif step == line - 2:
            relay(1, 0, True)

    @pl.loop(0, length // SPAN)
    def _(span):
        taken = pl.ds(pl.multiple_of(span * SPAN, SPAN), SPAN)
        for g, narrow, own in plans:
            lanes, mine = slice(g * 128, (g + 1) * 128), slice(own * 128, (own + 1) * 128)
            grown = jnp.exp(earlier_lanes[pl.ds(pl.multiple_of(span * 8, 8), 8), lanes][0:1])
            entering = (prefix[g] * grown + carried[span, g]).astype(half)
            across = dot(turned[taken, lanes], entering, 1, 0) * jnp.exp(cum_lanes[taken, lanes])
            output = within[taken, lanes] + across
            square = output * output
            if narrow:
                gate = narrow_gate[taken, mine].astype(jnp.float32)
                first = jnp.sum(jnp.where(low_half, square, 0.0), axis=-1, keepdims=True)
                second = jnp.sum(jnp.where(low_half, 0.0, square), axis=-1, keepdims=True)
                mean = jnp.where(low_half, first, second) * (1.0 / NARROW_DIM)
            else:
                gate = wide_gate[taken, mine].astype(jnp.float32)
                mean = jnp.mean(square, axis=-1, keepdims=True)
            normed = output * lax.rsqrt(mean + epsilon)
            mixed[taken, lanes] = (normed * (gate / (1.0 + jnp.exp(-gate)))).astype(half)

    wide_lanes = wide_groups * 128

    def project(start):
        taken = pl.ds(pl.multiple_of(start * block_rows, block_rows), block_rows)
        return jnp.dot(
            mixed[taken, :wide_lanes], wide_out[...], preferred_element_type=jnp.float32
        ) + jnp.dot(mixed[taken, wide_lanes:], narrow_out[...], preferred_element_type=jnp.float32)

    def part_copy(offset):
        return remote(
            part_out.at[offset], part_in.at[offset],
            part_send.at[offset], part_recv.at[offset], peer(offset),
        )

    @pl.loop(1, count_tp)
    def _(offset):
        part_out[offset] = project(lax.rem(tp + offset, count_tp)).astype(half)
        part_copy(offset).start()

    lowered[...] = project(tp)
    relay(1, 1, False)
    for offset in range(1, count_tp):
        part_copy(offset).wait_recv()
        lowered[...] += part_in[offset].astype(jnp.float32)

    mine = pl.ds(pl.multiple_of(tp * block_rows, block_rows), block_rows)
    moved = residual[...].astype(jnp.float32) + rms_scale(lowered[...], gain_mix[...])
    moved = moved.astype(half)
    updated[...] = moved
    rows[mine, :] = rms_scale(moved.astype(jnp.float32), gain_pre[...]).astype(half)

    def row_copy(offset):
        return remote(
            rows.at[mine], rows.at[mine], row_send.at[offset], row_recv.at[offset], peer(offset)
        )

    for offset in range(1, count_tp):
        row_copy(offset).start()
    for place in range(line):
        wait_pair(0, place)
    for offset in range(1, count_tp):
        row_copy(offset).wait_recv()

    width = 256

    @pl.loop(0, hidden.shape[1] // width)
    def _(tile):
        taken = pl.ds(pl.multiple_of(tile * width, width), width)
        total = jnp.zeros((length, width), jnp.float32)
        for block in range(count_sp):
            total += jnp.dot(
                rows[:, block * slab : (block + 1) * slab], up_slots[block, :, taken],
                preferred_element_type=jnp.float32,
            )
        rectified = jax.nn.relu(total)
        hidden[:, taken] = (rectified * rectified).astype(half)

    def low_copy(offset, block):
        start = lax.rem(tp + offset, count_tp) * block_rows
        return remote(
            low_out.at[block, pl.ds(pl.multiple_of(start, block_rows), block_rows)],
            low_in.at[offset, block],
            low_send.at[offset, block], low_recv.at[offset, block], peer(offset),
        )

    def consume(block):
        low_out[block] = jnp.dot(
            hidden[...], down_slots[block], preferred_element_type=jnp.float32
        ).astype(half)
        for offset in range(1, count_tp):
            low_copy(offset, block).start()

    def at_distance(act, distance):
        @pl.when(a - distance >= 0)
        def _():
            act(a - distance)

        @pl.when((a + distance < line) & (distance > 0))
        def _():
            act(a + distance)

    def from_pair(place):
        wait_pair(1, place)
        consume(place * 2 + 1 - b)

    @pl.loop(0, line)
    def _(distance):
        @pl.when((distance + 1 <= line - 2) & (distance > 0))
        def _():
            relay(1, distance + 1, False)

        at_distance(lambda place: consume(place * 2 + b), distance)
        at_distance(from_pair, distance)

    for block in range(count_sp):
        taken = slice(block * columns, (block + 1) * columns)
        total = low_out[block, mine, :].astype(jnp.float32)
        for offset in range(1, count_tp):
            low_copy(offset, block).wait_recv()
            total += low_in[offset, block].astype(jnp.float32)
        lowered[:, taken] = total
    result[...] = (
        updated[...].astype(jnp.float32) + rms_scale(lowered[...], gain_mlp[...])
    ).astype(half)

    for offset in range(1, count_tp):
        part_copy(offset).wait_send()
        row_copy(offset).wait_send()

        @pl.loop(0, count_sp)
        def _(block):
            low_copy(offset, block).wait_send()

    for step in range(len(distances)):
        @pl.when(sp + distances[step] < count_sp)
        def _():
            for copy in state_copies(step):
                copy.wait_send()

    for which in range(2):
        swap_copy(which, a).wait_send()
        for index in range(PIECES):
            @pl.loop(0, line)
            def _(place):
                if index == 0:
                    pair_copy(which, index, place, b).wait_send()
                else:
                    @pl.when(place != twin)
                    def _():
                        pair_copy(which, index, place, b).wait_send()

            @pl.loop(0, line - 1)
            def _(step):
                @pl.when((a + 1 < line) & (a - step >= 0))
                def _():
                    right_copy(which, step, index, jnp.maximum(a - step, 0)).wait_send()

                @pl.when((a >= 1) & (a + step < line))
                def _():
                    left_copy(which, step, index, jnp.minimum(a + step, line - 1)).wait_send()


def turn_tables(head_dim, positions):
    lane = jnp.arange(128, dtype=jnp.int32) % head_dim
    half = head_dim // 2
    pair = (lane % half).astype(jnp.float32) * 2.0
    inverse = 10000.0 ** (-pair / head_dim)
    angles = positions.astype(jnp.float32)[:, None] * inverse[None, :]
    return jnp.cos(angles), jnp.where(lane < half, -1.0, 1.0)[None, :] * jnp.sin(angles)


def whole_call(
    wide, narrow, wide_decay, narrow_decay, residual, wide_out, narrow_out,
    up_weight, down_weight, gain_mix, gain_pre, gain_mlp, count_sp, count_tp,
):
    block_rows, features = residual.shape
    length = wide[0].shape[0]
    spans = length // SPAN
    slab, inner = up_weight.shape
    depth, columns = down_weight.shape
    wide_groups, narrow_groups = wide[0].shape[1] // 128, narrow[0].shape[1] // 128
    groups = wide_groups + narrow_groups
    positions = lax.axis_index("sp") * length + jnp.arange(length, dtype=jnp.int32)
    tables = jnp.stack([*turn_tables(WIDE_DIM, positions), *turn_tables(NARROW_DIM, positions)])
    decay = jnp.concatenate([wide_decay, narrow_decay], axis=0)
    heads = decay.shape[0]
    cumulative = jnp.cumsum(decay.reshape(heads, spans, SPAN), axis=-1)
    cum_rows = cumulative.reshape(heads, length)
    widths = [WIDE_DIM] * wide_decay.shape[0] + [NARROW_DIM] * narrow_decay.shape[0]

    def over_lanes(values):
        return jnp.concatenate(
            [
                jnp.broadcast_to(values[:, h : h + 1], (values.shape[0], width))
                for h, width in enumerate(widths)
            ],
            axis=1,
        )

    totals = cumulative[:, :, -1].T
    earlier = jnp.cumsum(totals, axis=0) - totals
    device = jnp.exp(jnp.sum(totals, axis=0, keepdims=True))
    half, full, line = jnp.bfloat16, jnp.float32, count_sp // 2
    steps = (count_sp - 1).bit_length()
    tall = -(-groups // 8) * 8
    dma = pltpu.SemaphoreType.DMA
    vmem = pl.BlockSpec(memory_space=pltpu.VMEM)
    anywhere = pl.BlockSpec(memory_space=pl.ANY)
    return pl.pallas_call(
        functools.partial(whole_kernel, count_sp, count_tp, wide_groups, narrow_groups),
        out_shape=jax.ShapeDtypeStruct(residual.shape, half),
        in_specs=[vmem] * 20 + [anywhere] * 2,
        out_specs=vmem,
        scratch_shapes=[
            pltpu.VMEM((count_sp, slab, inner), half),
            pltpu.VMEM((count_sp, depth, columns), half),
            pltpu.VMEM((count_tp, block_rows, features), half),
            pltpu.VMEM((count_tp, block_rows, features), half),
            pltpu.VMEM((length, features), half),
            pltpu.VMEM((length, depth), half),
            pltpu.VMEM((count_sp, length, columns), half),
            pltpu.VMEM((count_tp, count_sp, block_rows, columns), half),
            pltpu.VMEM((block_rows, features), half),
            pltpu.VMEM((block_rows, features), full),
            pltpu.VMEM((length, groups * 128), half),
            pltpu.VMEM((length, groups * 128), full),
            pltpu.VMEM((spans, groups, 128, 128), full),
            pltpu.VMEM((length, groups * 128), half),
            pltpu.VMEM((groups, 128, 128), full),
            pltpu.VMEM((groups, 128, 128), full),
            pltpu.VMEM((tall, 128), full),
            pltpu.VMEM((steps, groups, 128, 128), half),
            pltpu.VMEM((steps, groups, 128, 128), half),
            pltpu.VMEM((steps, tall, 128), full),
            pltpu.VMEM((steps, tall, 128), full),
            dma((2, 2, line - 1, PIECES)),
            dma((2, 2, line - 1, PIECES)),
            dma((2, line, PIECES)),
            dma((2, line, PIECES)),
            dma((2,)),
            dma((2,)),
            dma((count_tp,)),
            dma((count_tp,)),
            dma((count_tp,)),
            dma((count_tp,)),
            dma((count_tp, count_sp)),
            dma((count_tp, count_sp)),
            dma((steps,)),
            dma((steps,)),
            dma((steps,)),
            dma((steps,)),
            dma((2,)),
        ],
        compiler_params=pltpu.CompilerParams(
            collective_id=0, has_side_effects=True, vmem_limit_bytes=58 * 1024 * 1024
        ),
    )(
        *wide, *narrow, tables, cum_rows, over_lanes(cum_rows.T),
        jnp.repeat(over_lanes(totals), 8, axis=0), jnp.repeat(over_lanes(earlier), 8, axis=0),
        over_lanes(device), residual, wide_out, narrow_out,
        gain_mix[None, :], gain_pre[None, :], gain_mlp[None, :], up_weight, down_weight,
    )


def solution(mesh):
    return jax.shard_map(
        local,
        mesh=mesh,
        in_specs=(
            P("sp", "tp"),
            P("sp", "tp"),
            P("sp", "tp"),
            P("sp", "tp"),
            P("sp", "tp"),
            P("sp", "tp"),
            P("sp", "tp"),
            P("sp", "tp"),
            P("tp", "sp"),
            P("tp", "sp"),
            P(("sp", "tp"), None),
            P("tp", None),
            P("tp", None),
            P("sp", "tp"),
            P("tp", "sp"),
            P(),
            P(),
            P(),
        ),
        out_specs=P(("sp", "tp"), None),
        check_vma=False,
    )
```

```python
import functools

import jax
import jax.numpy as jnp
from jax import lax
from jax.experimental import pallas as pl
from jax.experimental.pallas import tpu as pltpu
from jax.sharding import PartitionSpec as P

MESH = pl.DeviceIdType.MESH

WIDE_DIM = 128
NARROW_DIM = 64
SPAN = 128


epsilon = 1e-06


def pack_states(items):
    wide_decay, wide_state, narrow_decay, narrow_state = items
    decays = jnp.concatenate([wide_decay, narrow_decay])
    decays = jnp.pad(decays[None, :], ((0, 15), (0, 128 - decays.shape[0])))
    return jnp.concatenate(
        [wide_state.reshape(-1, 128), narrow_state.reshape(-1, 128), decays], axis=0
    ).astype(jnp.bfloat16)


def unpack_states(packed, like):
    packed = packed.astype(jnp.float32)
    wide_rows, narrow_rows = like[1].size // 128, like[3].size // 128
    decays = packed[wide_rows + narrow_rows]
    wide_heads, narrow_heads = like[0].shape[0], like[2].shape[0]
    return (
        decays[:wide_heads],
        packed[:wide_rows].reshape(like[1].shape),
        decays[wide_heads : wide_heads + narrow_heads],
        packed[wide_rows : wide_rows + narrow_rows].reshape(like[3].shape),
    )


def earlier_states(own, axis, count):
    whole, before, distance = own, None, 1
    while distance < count:
        arrived = lax.ppermute(
            pack_states(whole), axis, [(i, i + distance) for i in range(count - distance)]
        )
        arrived = unpack_states(arrived, own)
        before = arrived if before is None else combine_states(arrived, before)
        whole = combine_states(arrived, whole)
        distance *= 2
    return before


def rotate(packed, head_dim, positions):
    length = packed.shape[0]
    grouped = packed.astype(jnp.float32).reshape(length, -1, head_dim)
    halfway = head_dim // 2
    inverse = 10000.0 ** (-jnp.arange(0, head_dim, 2, dtype=jnp.float32) / head_dim)
    angles = positions.astype(jnp.float32)[:, None] * inverse[None, :]
    cosine_table = jnp.cos(angles)[:, None, :]
    sine_table = jnp.sin(angles)[:, None, :]
    leading = grouped[..., :halfway]
    trailing = grouped[..., halfway:]
    return jnp.concatenate(
        [
            leading * cosine_table - trailing * sine_table,
            leading * sine_table + trailing * cosine_table,
        ],
        axis=-1,
    )


def rms_scale(values, gain_vector):
    return (
        values
        * lax.rsqrt(jnp.mean(values * values, axis=-1, keepdims=True) + epsilon)
        * gain_vector
    )


def span_terms(query, key, value, log_decay, head_dim, offset):
    length = query.shape[0]
    count_of_heads = query.shape[1] // head_dim
    span_count = length // SPAN
    shaped = (span_count, SPAN, count_of_heads, head_dim)
    positions = offset + jnp.arange(length, dtype=jnp.int32)
    queries = rotate(query, head_dim, positions).astype(jnp.bfloat16).reshape(shaped)
    keys_full = (rotate(key, head_dim, positions) * head_dim ** (-0.5)).reshape(shaped)
    keys_half = keys_full.astype(jnp.bfloat16)
    values_all = value.reshape(shaped)
    cumulative = jnp.cumsum(log_decay.T.reshape(span_count, SPAN, count_of_heads), axis=1)
    causal = jnp.arange(SPAN)[:, None] >= jnp.arange(SPAN)[None, :]
    scores = jnp.einsum("nihd,njhd->nhij", queries, keys_half, preferred_element_type=jnp.float32)
    decay_rows = cumulative.transpose(0, 2, 1)
    log_gaps = jnp.where(causal, decay_rows[..., :, None] - decay_rows[..., None, :], -jnp.inf)
    weights = (scores * jnp.exp(log_gaps)).astype(jnp.bfloat16)
    within = jnp.einsum("nhij,njhd->nihd", weights, values_all, preferred_element_type=jnp.float32)
    span_total = cumulative[:, -1, :]
    scaled = (keys_full * jnp.exp(span_total[:, None, :] - cumulative)[..., None]).astype(
        jnp.bfloat16
    )
    own_state = jnp.einsum(
        "njhd,njhe->nhde", scaled, values_all, preferred_element_type=jnp.float32
    )

    def advance(carried, inputs):
        decay_sum, contribution = inputs
        return (carried * jnp.exp(decay_sum)[:, None, None] + contribution, carried)

    initial = jnp.zeros((count_of_heads, head_dim, head_dim), jnp.float32)
    closing, before = lax.scan(advance, initial, (span_total, own_state), unroll=True)
    device_decay = jnp.exp(jnp.sum(span_total, axis=0))
    return (queries, cumulative, within, span_total, before, closing, device_decay)


def finish(parts, prefix, gate, head_dim):
    queries, cumulative, within, span_total, before, closing, device_decay = parts
    length = gate.shape[0]
    earlier = jnp.cumsum(span_total, axis=0) - span_total
    entering = (prefix[None] * jnp.exp(earlier)[:, :, None, None] + before).astype(jnp.bfloat16)
    across = (
        jnp.einsum("nihd,nhde->nihe", queries, entering, preferred_element_type=jnp.float32)
        * jnp.exp(cumulative)[..., None]
    )
    output = (within + across).reshape(length, -1, head_dim)
    normed = output * lax.rsqrt(jnp.mean(output * output, axis=-1, keepdims=True) + epsilon)
    return (normed.reshape(length, -1) * jax.nn.silu(gate.astype(jnp.float32))).astype(jnp.bfloat16)


def combine_states(former, latter):
    return (
        former[0] * latter[0],
        former[1] * latter[0][:, None, None] + latter[1],
        former[2] * latter[2],
        former[3] * latter[2][:, None, None] + latter[3],
    )


def local(
    wide_query,
    wide_key,
    wide_value,
    wide_gate,
    narrow_query,
    narrow_key,
    narrow_value,
    narrow_gate,
    wide_decay,
    narrow_decay,
    residual,
    wide_out,
    narrow_out,
    up_weight,
    down_weight,
    gain_mix,
    gain_pre,
    gain_mlp,
):
    columns = down_weight.shape[1]
    count_sp, count_tp = lax.axis_size("sp"), lax.axis_size("tp")
    if (
        columns % 128 == 0 and count_sp % 4 == 0 and count_sp >= 8 and count_tp > 1
        and narrow_query.shape[1] % 128 == 0
    ):
        return whole_call(
            (wide_query, wide_key, wide_value, wide_gate),
            (narrow_query, narrow_key, narrow_value, narrow_gate),
            wide_decay, narrow_decay, residual, wide_out, narrow_out,
            up_weight, down_weight, gain_mix, gain_pre, gain_mlp, count_sp, count_tp,
        )
    length = wide_query.shape[0]
    offset = lax.axis_index("sp") * length
    wide_parts = span_terms(wide_query, wide_key, wide_value, wide_decay, WIDE_DIM, offset)
    narrow_parts = span_terms(
        narrow_query, narrow_key, narrow_value, narrow_decay, NARROW_DIM, offset
    )
    prefixes = earlier_states(
        (wide_parts[6], wide_parts[5], narrow_parts[6], narrow_parts[5]),
        "sp",
        lax.axis_size("sp"),
    )
    wide_mixed = finish(wide_parts, prefixes[1], wide_gate, WIDE_DIM)
    narrow_mixed = finish(narrow_parts, prefixes[3], narrow_gate, NARROW_DIM)
    return tail_plain(
        wide_mixed, narrow_mixed, wide_out, narrow_out, residual,
        gain_mix, gain_pre, gain_mlp, up_weight, down_weight,
    )


def tail_plain(
    wide_mixed, narrow_mixed, wide_out, narrow_out, residual,
    gain_mix, gain_pre, gain_mlp, up_weight, down_weight,
):
    wide_rows, narrow_rows = (
        lax.all_to_all(wide_mixed, "tp", split_axis=0, concat_axis=1, tiled=True),
        lax.all_to_all(narrow_mixed, "tp", split_axis=0, concat_axis=1, tiled=True),
    )
    wide_whole, narrow_whole = (
        lax.all_gather(wide_out, "tp", axis=0, tiled=True),
        lax.all_gather(narrow_out, "tp", axis=0, tiled=True),
    )
    projected = jnp.dot(wide_rows, wide_whole, preferred_element_type=jnp.float32) + jnp.dot(
        narrow_rows, narrow_whole, preferred_element_type=jnp.float32
    )
    updated = (residual.astype(jnp.float32) + rms_scale(projected, gain_mix)).astype(jnp.bfloat16)
    normed = rms_scale(updated.astype(jnp.float32), gain_pre).astype(jnp.bfloat16)
    block_rows = lax.all_gather(normed, "tp", axis=0, tiled=True)
    rectified = jax.nn.relu(
        jnp.dot(
            block_rows,
            lax.all_gather(up_weight, "sp", axis=0, tiled=True),
            preferred_element_type=jnp.float32,
        )
    )
    hidden = (rectified * rectified).astype(jnp.bfloat16)
    partial_terms = jnp.dot(
        hidden,
        lax.all_gather(down_weight, "sp", axis=1, tiled=True),
        preferred_element_type=jnp.float32,
    )
    lowered = lax.psum_scatter(
        partial_terms.astype(jnp.bfloat16), "tp", scatter_dimension=0, tiled=True
    ).astype(jnp.float32)
    return (updated.astype(jnp.float32) + rms_scale(lowered, gain_mlp)).astype(jnp.bfloat16)


PIECES = 2


def swap_halves(values, head_dim):
    half = head_dim // 2
    if head_dim == 128:
        return pltpu.roll(values, half, 1)
    lane = lax.broadcasted_iota(jnp.int32, values.shape, 1)
    return jnp.where(
        lax.rem(lane, head_dim) < half,
        pltpu.roll(values, 128 - half, 1),
        pltpu.roll(values, half, 1),
    )


def whole_kernel(
    count_sp, count_tp, wide_groups, narrow_groups,
    wide_query, wide_key, wide_value, wide_gate,
    narrow_query, narrow_key, narrow_value, narrow_gate,
    tables, cum_rows, cum_lanes, total_lanes, earlier_lanes, device_lanes,
    residual, wide_out, narrow_out, gain_mix, gain_pre, gain_mlp, up_hbm, down_hbm,
    result,
    up_slots, down_slots, part_out, part_in, rows, hidden, low_out, low_in, updated, lowered,
    turned, within, carried, mixed, state, prefix, prefix_decay, state_out, state_in,
    decay_out, decay_in,
    line_send, line_recv, pair_send, pair_recv, swap_send, swap_recv, part_send, part_recv,
    row_send, row_recv, low_send, low_recv, state_send, state_recv, decay_send, decay_recv,
    local_sem,
):
    line = count_sp // 2
    groups = wide_groups + narrow_groups
    sp, tp = lax.axis_index("sp"), lax.axis_index("tp")
    a, b = sp // 2, lax.rem(sp, 2)
    twin = a + 1 - 2 * lax.rem(a, 2)
    block_rows = residual.shape[0]
    length, features = rows.shape
    slots = (up_slots, down_slots)
    depth, columns = down_slots.shape[1], down_slots.shape[2]
    slab = up_slots.shape[1]
    half = jnp.bfloat16
    distances = []
    while 2 ** len(distances) < count_sp:
        distances.append(2 ** len(distances))

    def at(line_place, pair_place):
        return (line_place * 2 + pair_place, tp)

    def peer(offset):
        return (sp, lax.rem(tp + offset, count_tp))

    own_up = pltpu.make_async_copy(up_hbm, up_slots.at[sp], local_sem.at[0])
    own_up.start()
    own_down = pltpu.make_async_copy(down_hbm, down_slots.at[sp], local_sem.at[1])
    own_down.start()

    barrier = pltpu.get_barrier_semaphore()
    greeted = [at(a, 1 - b)]
    greeted += [(lax.rem(sp + step, count_sp), tp) for step in distances]
    greeted += [(lax.rem(sp + count_sp - step, count_sp), tp) for step in distances]
    greeted += [peer(offset) for offset in range(1, count_tp)]
    for other in greeted:
        pl.semaphore_signal(barrier, inc=1, device_id=other, device_id_type=MESH)
    pl.semaphore_wait(barrier, len(greeted))
    own_up.wait()
    own_down.wait()

    def chunk(which, place, index):
        piece = slots[which].shape[1] // PIECES
        return slots[which].at[place, pl.ds(index * piece, piece)]

    def remote(source, target, send, recv, device):
        return pltpu.make_async_remote_copy(
            src_ref=source, dst_ref=target, send_sem=send, recv_sem=recv,
            device_id=device, device_id_type=MESH,
        )

    def right_copy(which, step, index, place):
        ref = chunk(which, place * 2 + b, index)
        return remote(
            ref, ref, line_send.at[which, 0, step, index], line_recv.at[which, 0, step, index],
            at(jnp.minimum(a + 1, line - 1), b),
        )

    def left_copy(which, step, index, place):
        ref = chunk(which, place * 2 + b, index)
        return remote(
            ref, ref, line_send.at[which, 1, step, index], line_recv.at[which, 1, step, index],
            at(jnp.maximum(a - 1, 0), b),
        )

    def pair_copy(which, index, place, column):
        ref = chunk(which, place * 2 + column, index)
        return remote(
            ref, ref, pair_send.at[which, place, index], pair_recv.at[which, place, index],
            at(a, 1 - b),
        )

    def swap_copy(which, place):
        ref = chunk(which, place * 2 + 1 - b, 1)
        return remote(ref, ref, swap_send.at[which], swap_recv.at[which], at(twin, b))

    def begin(which):
        for index in range(PIECES):
            @pl.when(a + 1 < line)
            def _():
                right_copy(which, 0, index, a).start()

            @pl.when(a >= 1)
            def _():
                left_copy(which, 0, index, a).start()

            pair_copy(which, index, a, b).start()

    def to_pair(which, index, place):
        if index == 0:
            pair_copy(which, index, place, b).start()
        else:
            @pl.when(place != twin)
            def _():
                pair_copy(which, index, place, b).start()

    def relay(which, step, first):
        for index in range(PIECES):
            @pl.when(a - 1 - step >= 0)
            def _():
                place = a - 1 - step
                right_copy(which, step, index, place).wait_recv()

                @pl.when((a + 1 < line) & (step < line - 2))
                def _():
                    right_copy(which, jnp.minimum(step + 1, line - 2), index, place).start()

                to_pair(which, index, place)

            @pl.when(a + 1 + step < line)
            def _():
                place = a + 1 + step
                left_copy(which, step, index, place).wait_recv()

                @pl.when((a >= 1) & (step < line - 2))
                def _():
                    left_copy(which, jnp.minimum(step + 1, line - 2), index, place).start()

                to_pair(which, index, place)

        if first:
            pair_copy(which, 1, a, 1 - b).wait_recv()
            swap_copy(which, a).start()

    def wait_pair(which, place):
        pair_copy(which, 0, place, 1 - b).wait_recv()

        @pl.when((place != a) & (place != twin))
        def _():
            pair_copy(which, 1, place, 1 - b).wait_recv()

        @pl.when(place == twin)
        def _():
            swap_copy(which, place).wait_recv()

    begin(0)

    lane = lax.broadcasted_iota(jnp.int32, (SPAN, 128), 1)
    position = lax.broadcasted_iota(jnp.int32, (SPAN, 128), 0)
    causal = position >= lane
    low_half = lane < 64
    same_head = low_half == (position < 64)
    plans = [(g, False, g) for g in range(wide_groups)]
    plans += [(wide_groups + g, True, g) for g in range(narrow_groups)]

    def dot(left, right, left_dim, right_dim):
        return lax.dot_general(
            left, right, (((left_dim,), (right_dim,)), ((), ())),
            preferred_element_type=jnp.float32,
        )

    for g in range(groups):
        state[g] = jnp.zeros((128, 128), jnp.float32)

    @pl.loop(0, length // SPAN)
    def _(span):
        taken = pl.ds(pl.multiple_of(span * SPAN, SPAN), SPAN)
        for g, narrow, own in plans:
            lanes, mine = slice(g * 128, (g + 1) * 128), slice(own * 128, (own + 1) * 128)
            if narrow:
                query, key, value = narrow_query, narrow_key, narrow_value
                head_dim, cosine, sine = NARROW_DIM, tables[2, taken, :], tables[3, taken, :]
            else:
                query, key, value = wide_query, wide_key, wide_value
                head_dim, cosine, sine = WIDE_DIM, tables[0, taken, :], tables[1, taken, :]
            raw = query[taken, mine].astype(jnp.float32)
            spun = (raw * cosine + swap_halves(raw, head_dim) * sine).astype(half)
            turned[taken, lanes] = spun
            raw = key[taken, mine].astype(jnp.float32)
            full = (raw * cosine + swap_halves(raw, head_dim) * sine) * head_dim ** (-0.5)
            keys = full.astype(half)
            values = value[taken, mine]
            sums = cum_lanes[taken, lanes]
            total = total_lanes[pl.ds(pl.multiple_of(span * 8, 8), 8), lanes][0:1]

            def attend(queries, column, head):
                gaps = jnp.where(causal, column - cum_rows[head : head + 1, taken], -jnp.inf)
                weights = (dot(queries, keys, 1, 1) * jnp.exp(gaps)).astype(half)
                return dot(weights, values, 1, 0)

            if narrow:
                head = wide_groups + 2 * own
                first = attend(jnp.where(low_half, spun, jnp.zeros_like(spun)), sums[:, 0:1], head)
                second = attend(
                    jnp.where(low_half, jnp.zeros_like(spun), spun), sums[:, 64:65], head + 1
                )
                within[taken, lanes] = jnp.where(low_half, first, second)
            else:
                within[taken, lanes] = attend(spun, sums, g)
            scaled = (full * jnp.exp(total - sums)).astype(half)
            update = dot(scaled, values, 0, 0)
            if narrow:
                update = jnp.where(same_head, update, 0.0)
            old = state[g]
            carried[span, g] = old
            state[g] = old * jnp.exp(total) + update

    prefix[...] = jnp.zeros_like(prefix)
    prefix_decay[...] = jnp.ones_like(prefix_decay)

    def state_copies(step):
        device = (lax.rem(sp + distances[step], count_sp), tp)
        return (
            remote(
                state_out.at[step], state_in.at[step],
                state_send.at[step], state_recv.at[step], device,
            ),
            remote(
                decay_out.at[step], decay_in.at[step],
                decay_send.at[step], decay_recv.at[step], device,
            ),
        )

    def send_state(step):
        @pl.when(sp + distances[step] < count_sp)
        def _():
            for copy in state_copies(step):
                copy.start()

    def take_state(step):
        @pl.when(sp >= distances[step])
        def _():
            for copy in state_copies(step):
                copy.wait_recv()
            for g in range(groups):
                arrived = state_in[step, g].astype(jnp.float32)
                decay = decay_in[step, g : g + 1, :]
                prefix[g] = arrived * prefix_decay[g : g + 1, :] + prefix[g]
                prefix_decay[g : g + 1, :] = decay * prefix_decay[g : g + 1, :]
                if step + 1 < len(distances):
                    mine = decay_out[step, g : g + 1, :]
                    state[g] = arrived * mine + state[g]
                    decay_out[step + 1, g : g + 1, :] = decay * mine
                    state_out[step + 1, g] = state[g].astype(half)

        if step + 1 < len(distances):
            @pl.when(sp < distances[step])
            def _():
                decay_out[step + 1] = decay_out[step]
                for g in range(groups):
                    state_out[step + 1, g] = state[g].astype(half)

            send_state(step + 1)

    decay_out[0] = jnp.ones_like(decay_out[0])
    for g in range(groups):
        decay_out[0, g : g + 1, :] = device_lanes[:, g * 128 : (g + 1) * 128]
        state_out[0, g] = state[g].astype(half)
    send_state(0)
    relay(0, 0, True)
    begin(1)
    for step in range(max(len(distances), line - 1)):
        if step < len(distances):
            take_state(step)
        if step + 1 <= line - 2:
            relay(0, step + 1, False)
        elif step == line - 2:
            relay(1, 0, True)

    @pl.loop(0, length // SPAN)
    def _(span):
        taken = pl.ds(pl.multiple_of(span * SPAN, SPAN), SPAN)
        for g, narrow, own in plans:
            lanes, mine = slice(g * 128, (g + 1) * 128), slice(own * 128, (own + 1) * 128)
            grown = jnp.exp(earlier_lanes[pl.ds(pl.multiple_of(span * 8, 8), 8), lanes][0:1])
            entering = (prefix[g] * grown + carried[span, g]).astype(half)
            across = dot(turned[taken, lanes], entering, 1, 0) * jnp.exp(cum_lanes[taken, lanes])
            output = within[taken, lanes] + across
            square = output * output
            if narrow:
                gate = narrow_gate[taken, mine].astype(jnp.float32)
                first = jnp.sum(jnp.where(low_half, square, 0.0), axis=-1, keepdims=True)
                second = jnp.sum(jnp.where(low_half, 0.0, square), axis=-1, keepdims=True)
                mean = jnp.where(low_half, first, second) * (1.0 / NARROW_DIM)
            else:
                gate = wide_gate[taken, mine].astype(jnp.float32)
                mean = jnp.mean(square, axis=-1, keepdims=True)
            normed = output * lax.rsqrt(mean + epsilon)
            mixed[taken, lanes] = (normed * (gate / (1.0 + jnp.exp(-gate)))).astype(half)

    wide_lanes = wide_groups * 128

    def project(start):
        taken = pl.ds(pl.multiple_of(start * block_rows, block_rows), block_rows)
        return jnp.dot(
            mixed[taken, :wide_lanes], wide_out[...], preferred_element_type=jnp.float32
        ) + jnp.dot(mixed[taken, wide_lanes:], narrow_out[...], preferred_element_type=jnp.float32)

    def part_copy(offset):
        return remote(
            part_out.at[offset], part_in.at[offset],
            part_send.at[offset], part_recv.at[offset], peer(offset),
        )

    @pl.loop(1, count_tp)
    def _(offset):
        part_out[offset] = project(lax.rem(tp + offset, count_tp)).astype(half)
        part_copy(offset).start()

    lowered[...] = project(tp)
    relay(1, 1, False)
    for offset in range(1, count_tp):
        part_copy(offset).wait_recv()
        lowered[...] += part_in[offset].astype(jnp.float32)

    mine = pl.ds(pl.multiple_of(tp * block_rows, block_rows), block_rows)
    moved = residual[...].astype(jnp.float32) + rms_scale(lowered[...], gain_mix[...])
    moved = moved.astype(half)
    updated[...] = moved
    rows[mine, :] = rms_scale(moved.astype(jnp.float32), gain_pre[...]).astype(half)

    def row_copy(offset):
        return remote(
            rows.at[mine], rows.at[mine], row_send.at[offset], row_recv.at[offset], peer(offset)
        )

    for offset in range(1, count_tp):
        row_copy(offset).start()
    for place in range(line):
        wait_pair(0, place)
    for offset in range(1, count_tp):
        row_copy(offset).wait_recv()

    width = 256

    @pl.loop(0, hidden.shape[1] // width)
    def _(tile):
        taken = pl.ds(pl.multiple_of(tile * width, width), width)
        total = jnp.zeros((length, width), jnp.float32)
        for block in range(count_sp):
            total += jnp.dot(
                rows[:, block * slab : (block + 1) * slab], up_slots[block, :, taken],
                preferred_element_type=jnp.float32,
            )
        rectified = jax.nn.relu(total)
        hidden[:, taken] = (rectified * rectified).astype(half)

    def low_copy(offset, block):
        start = lax.rem(tp + offset, count_tp) * block_rows
        return remote(
            low_out.at[block, pl.ds(pl.multiple_of(start, block_rows), block_rows)],
            low_in.at[offset, block],
            low_send.at[offset, block], low_recv.at[offset, block], peer(offset),
        )

    def consume(block):
        low_out[block] = jnp.dot(
            hidden[...], down_slots[block], preferred_element_type=jnp.float32
        ).astype(half)
        for offset in range(1, count_tp):
            low_copy(offset, block).start()

    def at_distance(act, distance):
        @pl.when(a - distance >= 0)
        def _():
            act(a - distance)

        @pl.when((a + distance < line) & (distance > 0))
        def _():
            act(a + distance)

    def from_pair(place):
        wait_pair(1, place)
        consume(place * 2 + 1 - b)

    @pl.loop(0, line)
    def _(distance):
        @pl.when((distance + 1 <= line - 2) & (distance > 0))
        def _():
            relay(1, distance + 1, False)

        at_distance(lambda place: consume(place * 2 + b), distance)
        at_distance(from_pair, distance)

    for block in range(count_sp):
        taken = slice(block * columns, (block + 1) * columns)
        total = low_out[block, mine, :].astype(jnp.float32)
        for offset in range(1, count_tp):
            low_copy(offset, block).wait_recv()
            total += low_in[offset, block].astype(jnp.float32)
        lowered[:, taken] = total
    result[...] = (
        updated[...].astype(jnp.float32) + rms_scale(lowered[...], gain_mlp[...])
    ).astype(half)

    for offset in range(1, count_tp):
        part_copy(offset).wait_send()
        row_copy(offset).wait_send()

        @pl.loop(0, count_sp)
        def _(block):
            low_copy(offset, block).wait_send()

    for step in range(len(distances)):
        @pl.when(sp + distances[step] < count_sp)
        def _():
            for copy in state_copies(step):
                copy.wait_send()

    for which in range(2):
        swap_copy(which, a).wait_send()
        for index in range(PIECES):
            @pl.loop(0, line)
            def _(place):
                if index == 0:
                    pair_copy(which, index, place, b).wait_send()
                else:
                    @pl.when(place != twin)
                    def _():
                        pair_copy(which, index, place, b).wait_send()

            @pl.loop(0, line - 1)
            def _(step):
                @pl.when((a + 1 < line) & (a - step >= 0))
                def _():
                    right_copy(which, step, index, jnp.maximum(a - step, 0)).wait_send()

                @pl.when((a >= 1) & (a + step < line))
                def _():
                    left_copy(which, step, index, jnp.minimum(a + step, line - 1)).wait_send()


def turn_tables(head_dim, positions):
    lane = jnp.arange(128, dtype=jnp.int32) % head_dim
    half = head_dim // 2
    pair = (lane % half).astype(jnp.float32) * 2.0
    inverse = 10000.0 ** (-pair / head_dim)
    angles = positions.astype(jnp.float32)[:, None] * inverse[None, :]
    return jnp.cos(angles), jnp.where(lane < half, -1.0, 1.0)[None, :] * jnp.sin(angles)


def whole_call(
    wide, narrow, wide_decay, narrow_decay, residual, wide_out, narrow_out,
    up_weight, down_weight, gain_mix, gain_pre, gain_mlp, count_sp, count_tp,
):
    block_rows, features = residual.shape
    length = wide[0].shape[0]
    spans = length // SPAN
    slab, inner = up_weight.shape
    depth, columns = down_weight.shape
    wide_groups, narrow_groups = wide[0].shape[1] // 128, narrow[0].shape[1] // 128
    groups = wide_groups + narrow_groups
    positions = lax.axis_index("sp") * length + jnp.arange(length, dtype=jnp.int32)
    tables = jnp.stack([*turn_tables(WIDE_DIM, positions), *turn_tables(NARROW_DIM, positions)])
    decay = jnp.concatenate([wide_decay, narrow_decay], axis=0)
    heads = decay.shape[0]
    cumulative = jnp.cumsum(decay.reshape(heads, spans, SPAN), axis=-1)
    cum_rows = cumulative.reshape(heads, length)
    widths = [WIDE_DIM] * wide_decay.shape[0] + [NARROW_DIM] * narrow_decay.shape[0]

    owner = [h for h, width in enumerate(widths) for _ in range(width)]
    spread = (jnp.arange(heads)[:, None] == jnp.array(owner)[None, :]).astype(jnp.float32)

    def over_lanes(values):
        return jnp.dot(values, spread, precision=lax.Precision.HIGHEST)

    totals = cumulative[:, :, -1].T
    earlier = jnp.cumsum(totals, axis=0) - totals
    device = jnp.sum(totals, axis=0, keepdims=True)
    half, full, line = jnp.bfloat16, jnp.float32, count_sp // 2
    steps = (count_sp - 1).bit_length()
    tall = -(-groups // 8) * 8
    dma = pltpu.SemaphoreType.DMA
    vmem = pl.BlockSpec(memory_space=pltpu.VMEM)
    anywhere = pl.BlockSpec(memory_space=pl.ANY)
    return pl.pallas_call(
        functools.partial(whole_kernel, count_sp, count_tp, wide_groups, narrow_groups),
        out_shape=jax.ShapeDtypeStruct(residual.shape, half),
        in_specs=[vmem] * 20 + [anywhere] * 2,
        out_specs=vmem,
        scratch_shapes=[
            pltpu.VMEM((count_sp, slab, inner), half),
            pltpu.VMEM((count_sp, depth, columns), half),
            pltpu.VMEM((count_tp, block_rows, features), half),
            pltpu.VMEM((count_tp, block_rows, features), half),
            pltpu.VMEM((length, features), half),
            pltpu.VMEM((length, depth), half),
            pltpu.VMEM((count_sp, length, columns), half),
            pltpu.VMEM((count_tp, count_sp, block_rows, columns), half),
            pltpu.VMEM((block_rows, features), half),
            pltpu.VMEM((block_rows, features), full),
            pltpu.VMEM((length, groups * 128), half),
            pltpu.VMEM((length, groups * 128), full),
            pltpu.VMEM((spans, groups, 128, 128), full),
            pltpu.VMEM((length, groups * 128), half),
            pltpu.VMEM((groups, 128, 128), full),
            pltpu.VMEM((groups, 128, 128), full),
            pltpu.VMEM((tall, 128), full),
            pltpu.VMEM((steps, groups, 128, 128), half),
            pltpu.VMEM((steps, groups, 128, 128), half),
            pltpu.VMEM((steps, tall, 128), full),
            pltpu.VMEM((steps, tall, 128), full),
            dma((2, 2, line - 1, PIECES)),
            dma((2, 2, line - 1, PIECES)),
            dma((2, line, PIECES)),
            dma((2, line, PIECES)),
            dma((2,)),
            dma((2,)),
            dma((count_tp,)),
            dma((count_tp,)),
            dma((count_tp,)),
            dma((count_tp,)),
            dma((count_tp, count_sp)),
            dma((count_tp, count_sp)),
            dma((steps,)),
            dma((steps,)),
            dma((steps,)),
            dma((steps,)),
            dma((2,)),
        ],
        compiler_params=pltpu.CompilerParams(
            collective_id=0, has_side_effects=True, vmem_limit_bytes=58 * 1024 * 1024
        ),
    )(
        *wide, *narrow, tables, cum_rows, over_lanes(cum_rows.T),
        over_lanes(jnp.repeat(totals, 8, axis=0)), over_lanes(jnp.repeat(earlier, 8, axis=0)),
        jnp.exp(over_lanes(device)), residual, wide_out, narrow_out,
        gain_mix[None, :], gain_pre[None, :], gain_mlp[None, :], up_weight, down_weight,
    )


def solution(mesh):
    return jax.shard_map(
        local,
        mesh=mesh,
        in_specs=(
            P("sp", "tp"),
            P("sp", "tp"),
            P("sp", "tp"),
            P("sp", "tp"),
            P("sp", "tp"),
            P("sp", "tp"),
            P("sp", "tp"),
            P("sp", "tp"),
            P("tp", "sp"),
            P("tp", "sp"),
            P(("sp", "tp"), None),
            P("tp", None),
            P("tp", None),
            P("sp", "tp"),
            P("tp", "sp"),
            P(),
            P(),
            P(),
        ),
        out_specs=P(("sp", "tp"), None),
        check_vma=False,
    )
```
